256 devices in a mesh: ep: 64 (over z, x, core), tp: 4 (over y).
Axes of the slice: x: 4, y: 4, z: 8, core: 2. Of those that a mesh axis runs over, the one named last changes fastest.
Arguments:
- conv_input: bfloat16 [32768, 2048], P(('ep', 'tp')), may hold values from -6 to 6
- conv_kernel: float32 [31, 2048], replicated, may hold values from -1 to 1
- conv_gain: float32 [2048], replicated, may hold values from 0.1 to 1.9
- out_weight: bfloat16 [2048, 2048], P(None, 'tp'), may hold values from -0.125 to 0.125
- moe_input: bfloat16 [32768, 2048], P(('ep', 'tp')), may hold values from -6 to 6
- moe_gain: float32 [2048], replicated, may hold values from 0.1 to 1.9
- expert_gate: bfloat16 [64, 2048, 2048], P('ep', None, 'tp'), may hold values from -0.125 to 0.125
- expert_up: bfloat16 [64, 2048, 2048], P('ep', None, 'tp'), may hold values from -0.125 to 0.125
- expert_down: bfloat16 [64, 2048, 2048], P('ep', 'tp'), may hold values from -0.125 to 0.125
- shared_gate: bfloat16 [2048, 128], replicated, may hold values from -0.125 to 0.125
- shared_up: bfloat16 [2048, 128], replicated, may hold values from -0.125 to 0.125
- shared_down: bfloat16 [128, 2048], replicated, may hold values from -0.5 to 0.5
- expert_index: int32 [32768, 2], P('ep'), may hold values from 0 to 63, all different within a row; in each aligned block of 128 rows (0 to 127, 128 to 255, ...) at most 6 rows name the same one
- routing_weight: float32 [32768, 2], P(('ep', 'tp')), may hold values from 0.25 to 1.5
Outputs:
- conv_out: bfloat16 [32768, 2048], P('ep', 'tp')
- moe_out: bfloat16 [32768, 2048], P(('ep', 'tp'))
The draws below stay inside these ranges and needn't reach their ends.
Inputs may be any that keep to these rules, and one draw needn't show every extreme that they name: `expert_index`: each row names 2 different experts. In each aligned block of 128 rows no expert is named by more than 6 of the rows, and in some blocks one expert is named by exactly 6 rows.
All inputs are finite; a program needn't handle non-finite values.
Results may differ from the reference program's by a relative error of at most 0.009.
Values may be sent and summed in bfloat16 or wider, within the bound.
No kernel may reach another device: no remote copies, remote signals or barrier semaphores. Data moves between devices by JAX's collectives and lax.ppermute only.
A program may use at most 128 MiB of HBM per device.

```python
import math
import jax
import jax.numpy as jnp
import numpy as np
from jax import lax

D = 2048
FF = 2048
SHARED_FF = 128
TOPK = 2
KERNEL = 31
TOK_DEV_B = 128
TOKENS_A = 32768
TOKENS_B = 32768
EXPERTS = 64
SLOTS = 6
N_TP = 4


def level_of(key, dims, cuts, smallest, largest):
    def one(axis_at, blocks):
        heights = jax.random.uniform(jax.random.fold_in(jax.random.fold_in(key, 6), axis_at), (blocks,), jnp.float32, smallest / len(cuts), largest / len(cuts))
        return jnp.repeat(jnp.exp(heights), dims[axis_at] // blocks).reshape((-1,) + (1,) * (len(dims) - axis_at - 1))

    level = one(*cuts[0])
    for cut in cuts[1:]:
        level = level * one(*cut)
    return level


def shared_out(key, own, number, rows, number_of, top, limit, slope):
    sequence = jax.random.permutation(key, number_of)
    crowded, common = shares(number_of, rows * top, limit, slope, True), shares(number_of, rows * top, limit, slope, False)
    places = jnp.arange(number_of)

    def named(sizes, rotation):
        used = int((sizes > 0).sum())
        fixed = max(1, used // 4)
        moved = fixed + (places - fixed + rotation * (used - fixed)) % max(1, number_of - fixed)
        return jnp.zeros((number_of,), jnp.int32).at[sequence[jnp.where(places < fixed, places, moved)]].set(jnp.asarray(sizes, jnp.int32))

    sizes = jnp.where(number % 4 == 0, named(crowded, number // 4), named(common, number - number // 4 - 1))
    mixed = jax.random.permutation(jax.random.fold_in(own, 3), number_of)
    donor, receiver = mixed[0:number_of // 2 * 2:2], mixed[1:number_of // 2 * 2:2]
    slack = jnp.minimum(sizes[donor] - 1, limit - sizes[receiver]) // 2
    slack = jnp.where((donor == sequence[0]) | (receiver == sequence[0]) | (sizes[receiver] == 0), 0, jnp.maximum(slack, 0))
    moved = jax.random.randint(jax.random.fold_in(own, 4), (number_of // 2,), 0, 1 << 20) % (slack + 1)
    sizes = sizes.at[donor].add(-moved).at[receiver].add(moved)
    members = jnp.searchsorted(jnp.cumsum(sizes), jnp.arange(rows * top), side="right").astype(jnp.int32)
    grid = members.reshape(top, rows).T
    grid = grid[jax.random.permutation(jax.random.fold_in(own, 1), rows)]
    rotation = jax.random.randint(jax.random.fold_in(own, 2), (rows, 1), 0, top)
    return jnp.take_along_axis(grid, (jnp.arange(top)[None, :] + rotation) % top, axis=1)


def shares(count, total, bound, skew, full):
    weights = [(1 << 20) // math.isqrt(rank ** skew) + 1 for rank in range(1, count + 1)]
    largest = bound if full else min(bound, max(-(-total // count), total * weights[0] // sum(weights)))
    least = 1 if total - largest >= count - 1 else 0
    given, rest = [largest] + [least] * (count - 1), total - largest - least * (count - 1)
    while rest > 0:
        free = [i for i in range(1, count) if given[i] < largest] or [i for i in range(1, count) if given[i] < bound]
        pool, remaining = sum([weights[i] for i in free]), rest
        for i in free:
            addition = min(bound - given[i], max(1, remaining * weights[i] // pool), rest)
            given[i] = given[i] + addition
            rest = rest - addition
    return np.array(given)


def normal_values(key, extent, width, limit, split=(), kind=jnp.bfloat16):
    level = level_of(key, extent, split, -0.22, 0.18) if split else 1.0
    values = jax.random.normal(key, extent, jnp.float32) * width * level
    return jnp.minimum(jnp.maximum(values, -limit), limit).astype(kind)


def setup_inputs(seed: int = 0) -> dict:
    splits = jax.random.split(jax.random.key(seed), 15)
    conv_input = normal_values(splits[0], (TOKENS_A, D), 1.0, 6.0, ((0, 256),))
    conv_kernel = normal_values(splits[1], (KERNEL, D), KERNEL ** -0.5, 1.0, (), jnp.float32)
    conv_gain = jnp.clip(1.0 + 0.18 * jax.random.normal(splits[2], (D,), jnp.float32), 0.1, 1.9)
    out_weight = normal_values(splits[3], (D, D), D ** -0.5, 0.125, ((1, 4),))
    moe_input = normal_values(splits[4], (TOKENS_B, D), 1.0, 6.0, ((0, 256),))
    moe_gain = jnp.clip(1.0 + 0.18 * jax.random.normal(splits[5], (D,), jnp.float32), 0.1, 1.9)
    expert_gate = normal_values(splits[6], (EXPERTS, D, FF), D ** -0.5, 0.125, ((0, 64), (2, 4)))
    expert_up = normal_values(splits[7], (EXPERTS, D, FF), D ** -0.5, 0.125, ((0, 64), (2, 4)))
    expert_down = normal_values(splits[8], (EXPERTS, FF, D), FF ** -0.5, 0.125, ((0, 64), (1, 4)))
    shared_gate = normal_values(splits[9], (D, SHARED_FF), D ** -0.5, 0.125)
    shared_up = normal_values(splits[10], (D, SHARED_FF), D ** -0.5, 0.125)
    shared_down = normal_values(splits[11], (SHARED_FF, D), SHARED_FF ** -0.5, 0.5)
    expert_index_keys = jax.random.split(jax.random.fold_in(splits[12], 1), TOKENS_B // TOK_DEV_B)
    expert_index_turns = jax.random.permutation(jax.random.fold_in(splits[12], 3), TOKENS_B // TOK_DEV_B)
    expert_index = jax.vmap(lambda own, number: shared_out(jax.random.fold_in(splits[12], 2), own, number, TOK_DEV_B, EXPERTS, TOPK, SLOTS, 2))(expert_index_keys, expert_index_turns).reshape((TOKENS_B, TOPK))
    routing_weight = jnp.clip(0.25 + 1.25 * jax.random.uniform(splits[13], (TOKENS_B, TOPK), jnp.float32) ** level_of(splits[13], (TOKENS_B, TOPK), ((0, 256),), -0.2, 0.2), 0.25, 1.5)
    return dict(conv_input=conv_input, conv_kernel=conv_kernel, conv_gain=conv_gain, out_weight=out_weight, moe_input=moe_input, moe_gain=moe_gain, expert_gate=expert_gate, expert_up=expert_up, expert_down=expert_down, shared_gate=shared_gate, shared_up=shared_up, shared_down=shared_down, expert_index=expert_index, routing_weight=routing_weight)


NORM_EPS = 1e-05

def layer_scale(row_data, gain_vec):
    values = row_data.astype(jnp.float32)
    center = values - lax.optimization_barrier(jnp.mean(values, axis=-1, keepdims=True))
    spread = lax.optimization_barrier(jnp.mean(center * center, axis=-1, keepdims=True))
    return center * lax.rsqrt(spread + NORM_EPS) * gain_vec

def depthwise(padded, kernel, length):
    running = jnp.zeros((length, padded.shape[1]), jnp.float32)
    for offset in range(kernel.shape[0]):
        running = running + padded[offset:offset + length].astype(jnp.float32) * kernel[offset]
    return running

def slot_table(block_index, experts, slot_count):
    onehot = (block_index[:, :, None] == jnp.arange(experts, dtype=jnp.int32)[None, None, :]).astype(jnp.int32)
    before = jnp.cumsum(onehot, axis=1) - onehot
    position = lax.optimization_barrier(jnp.sum(before * onehot, axis=2))
    return (block_index * slot_count + position).astype(jnp.int32)

def reference(conv_input, conv_kernel, conv_gain, out_weight, moe_input, moe_gain, expert_gate, expert_up, expert_down, shared_gate, shared_up, shared_down, expert_index, routing_weight):
    length = conv_input.shape[0]
    padded = jnp.concatenate([jnp.zeros((KERNEL - 1, D), jnp.bfloat16), conv_input], axis=0)
    mixed_rows = depthwise(padded, conv_kernel, length)
    normed = jax.nn.silu(layer_scale(mixed_rows, conv_gain)).astype(jnp.bfloat16)
    conv_out = jnp.dot(normed, out_weight, preferred_element_type=jnp.float32).astype(jnp.bfloat16)
    normal = layer_scale(moe_input, moe_gain).astype(jnp.bfloat16)
    blocks = TOKENS_B // TOK_DEV_B
    entries = TOK_DEV_B * TOPK
    block_index = expert_index.reshape(blocks, entries)
    entry_slot = slot_table(block_index, EXPERTS, SLOTS)
    block_ids = jnp.arange(blocks, dtype=jnp.int32)[:, None]
    entry_row = block_ids * TOK_DEV_B + jnp.arange(entries, dtype=jnp.int32)[None, :] // TOPK
    slot_row = jnp.zeros((blocks, EXPERTS * SLOTS), jnp.int32).at[block_ids, entry_slot].set(entry_row)
    slot_weight = jnp.zeros((blocks, EXPERTS * SLOTS), jnp.float32).at[block_ids, entry_slot].set(routing_weight.reshape(blocks, entries))
    slot_row = slot_row.reshape(blocks, EXPERTS, SLOTS)
    slot_weight = slot_weight.reshape(blocks, EXPERTS, SLOTS)
    quarter = FF // N_TP

    def expert_step(running, expert_id):
        rows_of = lax.dynamic_index_in_dim(slot_row, expert_id, 1, keepdims=False).reshape(-1)
        weights = lax.dynamic_index_in_dim(slot_weight, expert_id, 1, keepdims=False).reshape(-1, 1)
        row_data = normal[rows_of]
        gate_proj = jnp.dot(row_data, expert_gate[expert_id], preferred_element_type=jnp.float32)
        up_proj = jnp.dot(row_data, expert_up[expert_id], preferred_element_type=jnp.float32)
        hidden = (jax.nn.silu(gate_proj) * up_proj).astype(jnp.bfloat16)
        down_all = expert_down[expert_id]
        summed = jnp.zeros((row_data.shape[0], D), jnp.float32)
        for index_q in range(N_TP):
            part_q = jnp.dot(hidden[:, index_q * quarter:(index_q + 1) * quarter], down_all[index_q * quarter:(index_q + 1) * quarter], preferred_element_type=jnp.float32).astype(jnp.bfloat16)
            summed = summed + lax.optimization_barrier(part_q).astype(jnp.float32)
        result = lax.optimization_barrier(summed.astype(jnp.bfloat16)).astype(jnp.float32)
        return (running.at[rows_of].add(weights * result), None)
    routed, _ = lax.scan(expert_step, jnp.zeros((TOKENS_B, D), jnp.float32), jnp.arange(EXPERTS, dtype=jnp.int32))
    shared_gate_proj = jnp.dot(normal, shared_gate, preferred_element_type=jnp.float32)
    shared_up_proj = jnp.dot(normal, shared_up, preferred_element_type=jnp.float32)
    shared_hidden = (jax.nn.silu(shared_gate_proj) * shared_up_proj).astype(jnp.bfloat16)
    shared_part = jnp.dot(shared_hidden, shared_down, preferred_element_type=jnp.float32)
    moe_out = (shared_part + routed).astype(jnp.bfloat16)
    return (conv_out, moe_out)
```

```python
import functools

import jax
import jax.numpy as jnp
from jax import lax
from jax.experimental import pallas as pl
from jax.experimental.pallas import tpu as pltpu
from jax.sharding import PartitionSpec as P

NORM_EPS = 1e-05
CHUNKS = 2
F32 = jnp.float32
BF16 = jnp.bfloat16


def vmem(count):
    return [pl.BlockSpec(memory_space=pltpu.VMEM) for _ in range(count)]


def mm(a, b):
    return jnp.dot(a, b, preferred_element_type=F32)


def dispatch_kernel(part, lanes, slots, tp_ref, x_ref, gain_ref, idx_ref, normal_ref, slot_ref, *rest):
    outs, stacked = rest[:-1], rest[-1]
    tokens, width = x_ref.shape
    pieces = width // lanes
    values = x_ref[...].astype(F32)
    center = values - jnp.mean(values, axis=-1, keepdims=True)
    spread = jnp.mean(center * center, axis=-1, keepdims=True)
    normal = (center * lax.rsqrt(spread + NORM_EPS) * gain_ref[...]).astype(BF16)
    normal_ref[...] = normal
    for q in range(pieces):
        stacked[q * tokens : (q + 1) * tokens, :] = normal[:, q * lanes : (q + 1) * lanes]
    start = pl.multiple_of(tp_ref[0] * tokens, tokens)
    named = idx_ref[:, pl.ds(start, tokens)].astype(F32)
    rows = [named[j : j + 1, :] for j in range(2)]
    down = lax.broadcasted_iota(jnp.int32, (tokens, tokens), 0)
    across = lax.broadcasted_iota(jnp.int32, (tokens, tokens), 1)
    cols = [jnp.sum(jnp.where(down == across, r, 0.0), axis=1, keepdims=True) for r in rows]
    seen = []
    for r in rows:
        same = jnp.where(cols[0] == r, 1.0, 0.0) + jnp.where(cols[1] == r, 1.0, 0.0)
        seen.append(jnp.sum(jnp.where(down < across, same, 0.0), axis=0, keepdims=True).astype(jnp.int32))
    named = [r.astype(jnp.int32) for r in rows]
    for j in range(2):
        slot_ref[j : j + 1, :] = named[j] * slots + seen[j]
    block = 256
    for k, out in enumerate(outs):
        targets = []
        for j in range(2):
            place = seen[j] - k * part
            base = named[j] * (pieces * part) + place
            inside = (place >= 0) & (place < part)
            targets.append(
                jnp.concatenate([jnp.where(inside, base + q * part, -1) for q in range(pieces)], axis=1)
            )
        for b in range(out.shape[0] // block):
            at = lax.broadcasted_iota(jnp.int32, (block, pieces * tokens), 0) + b * block
            hit = (at == targets[0]) | (at == targets[1])
            pick = jnp.where(hit, 1.0, 0.0).astype(BF16)
            out[b * block : (b + 1) * block, :] = mm(pick, stacked[...]).astype(BF16)


def dispatch(tp_index, x, gain, idx, chunks, slots, experts, lanes):
    tokens, width = x.shape
    part = slots // chunks
    pieces = width // lanes
    packed = jax.ShapeDtypeStruct((experts * pieces * part, lanes), BF16)
    out = pl.pallas_call(
        functools.partial(dispatch_kernel, part, lanes, slots),
        out_shape=[
            jax.ShapeDtypeStruct((tokens, width), BF16),
            jax.ShapeDtypeStruct((2, tokens), jnp.int32),
        ]
        + [packed] * chunks,
        in_specs=[pl.BlockSpec(memory_space=pltpu.SMEM)] + vmem(3),
        out_specs=vmem(2 + chunks),
        scratch_shapes=[pltpu.VMEM((pieces * tokens, lanes), BF16)],
        name="dispatch",
    )(tp_index, x, gain, idx)
    return out[0], out[1], out[2:]


def experts_kernel(block, own, back, ahead, far_a, far_b, perm, wg, wu, wd, out_own, send_p, send_m, keep_b, keep_a, x, y):
    lanes = own.shape[1]
    width = wd.shape[1]
    pieces = width // lanes
    rows = own.shape[0] // pieces
    half = rows // 2
    step = block // pieces
    at = 0
    for source in (own, back, ahead, far_a, far_b):
        for b in range(source.shape[0] // block):
            moved = mm(perm[...], source[b * block : (b + 1) * block, :]).astype(BF16)
            for q in range(pieces):
                x[at : at + step, q * lanes : (q + 1) * lanes] = moved[q * step : (q + 1) * step, :]
            at += step
    gate = mm(x[...], wg[...])
    up = mm(x[...], wu[...])
    hidden = (gate / (1.0 + jnp.exp(-gate)) * up).astype(BF16)
    y[...] = mm(hidden, wd[...]).astype(BF16)
    out_own[...] = y[0:rows, :]
    send_p[0:half, :] = y[3 * rows : 3 * rows + half, :]
    send_p[half:rows, :] = y[2 * rows + half : 3 * rows, :]
    send_m[0:half, :] = y[3 * rows + half : 4 * rows, :]
    send_m[half:rows, :] = y[rows : rows + half, :]
    keep_b[...] = y[2 * rows : 2 * rows + half, :]
    keep_a[...] = y[rows + half : 2 * rows, :]


def run_experts(pieces_in, perm, wg, wu, wd):
    own = pieces_in[0]
    width = wd.shape[1]
    rows = own.shape[0] * own.shape[1] // width
    full = jax.ShapeDtypeStruct((rows, width), BF16)
    half = jax.ShapeDtypeStruct((rows // 2, width), BF16)
    return pl.pallas_call(
        functools.partial(experts_kernel, perm.shape[0]),
        out_shape=[full, full, full, half, half],
        in_specs=vmem(9),
        out_specs=vmem(5),
        scratch_shapes=[pltpu.VMEM((4 * rows, width), BF16), pltpu.VMEM((4 * rows, width), BF16)],
        compiler_params=pltpu.CompilerParams(vmem_limit_bytes=48 * 1024 * 1024),
        cost_estimate=pl.CostEstimate(
            flops=2 * 4 * rows * width * wg.shape[1] * 3,
            transcendentals=4 * rows * wg.shape[1],
            bytes_accessed=6 * wg.size + 16 * rows * width,
        ),
        name="experts",
    )(*pieces_in, perm, wg, wu, wd)


def finish_kernel(block, own, got_p, got_m, last_p, last_m, perm_t, out, total):
    rows, width = own.shape
    half = rows // 2
    total[0:half, :] = (
        own[0:half, :].astype(F32) + last_p[...].astype(F32) + got_m[half:rows, :].astype(F32)
    ).astype(BF16)
    total[half:rows, :] = (
        own[half:rows, :].astype(F32) + last_m[...].astype(F32) + got_p[half:rows, :].astype(F32)
    ).astype(BF16)
    lanes = out.shape[1]
    pieces = width // lanes
    step = block // pieces
    for b in range(out.shape[0] // block):
        stacked = jnp.concatenate(
            [total[b * step : (b + 1) * step, q * lanes : (q + 1) * lanes] for q in range(pieces)], axis=0
        )
        out[b * block : (b + 1) * block, :] = mm(perm_t[...], stacked).astype(BF16)


def finish(own, got_p, got_m, last_p, last_m, perm_t, lanes):
    rows, width = own.shape
    return pl.pallas_call(
        functools.partial(finish_kernel, perm_t.shape[0]),
        out_shape=jax.ShapeDtypeStruct((rows * width // lanes, lanes), BF16),
        in_specs=vmem(6),
        out_specs=vmem(1)[0],
        scratch_shapes=[pltpu.VMEM((rows, width), BF16)],
        name="finish",
    )(own, got_p, got_m, last_p, last_m, perm_t)


def combine_kernel(chunk, part, slots, slot_ref, weight_ref, ret, acc, out):
    tokens, width = acc.shape
    lanes = ret.shape[1]
    pieces = width // lanes
    down = lax.broadcasted_iota(jnp.int32, (tokens, tokens), 0)
    across = lax.broadcasted_iota(jnp.int32, (tokens, tokens), 1)

    def column(row):
        return jnp.sum(jnp.where(down == across, row, 0.0), axis=1, keepdims=True)

    slot = [column(slot_ref[j : j + 1, :].astype(F32)).astype(jnp.int32) for j in range(2)]
    weight = [column(weight_ref[j : j + 1, :]) for j in range(2)]
    targets = []
    for j in range(2):
        expert = slot[j] // slots
        place = slot[j] - expert * slots - chunk * part
        inside = (place >= 0) & (place < part)
        targets.append(jnp.where(inside, expert * (pieces * part) + place, -width))
    at = lax.broadcasted_iota(jnp.int32, (tokens, ret.shape[0]), 1)
    for q in range(pieces):
        picks = [jnp.where(at == targets[j] + q * part, 1.0, 0.0).astype(BF16) for j in range(2)]
        found = mm(jnp.concatenate(picks, axis=0), ret[...])
        span = slice(q * lanes, (q + 1) * lanes)
        out[:, span] = (
            acc[:, span] + weight[0] * found[0:tokens, :] + weight[1] * found[tokens:, :]
        ).astype(out.dtype)


def combine(chunk, part, slots, slot_rows, weights, ret, acc, dtype):
    return pl.pallas_call(
        functools.partial(combine_kernel, chunk, part, slots),
        out_shape=jax.ShapeDtypeStruct(acc.shape, dtype),
        in_specs=vmem(4),
        out_specs=vmem(1)[0],
        name="combine",
    )(slot_rows, weights, ret, acc)


def shifted(block, axis, distance):
    size = lax.axis_size(axis)
    return lax.ppermute(block, axis, [(i, (i + distance) % size) for i in range(size)])


def passed_along(block, axis, distance):
    devices = range(lax.axis_size(axis))
    route = [(i - distance, i) for i in devices if i - distance in devices]
    return lax.ppermute(block, axis, route)


def layer_scale(row_data, gain_vec):
    values = row_data.astype(F32)
    center = values - jnp.mean(values, axis=-1, keepdims=True)
    spread = jnp.mean(center * center, axis=-1, keepdims=True)
    return center * lax.rsqrt(spread + NORM_EPS) * gain_vec


def depthwise(padded, kernel, length):
    running = jnp.zeros((length, padded.shape[1]), F32)
    for offset in range(kernel.shape[0]):
        running = running + padded[offset : offset + length].astype(F32) * kernel[offset]
    return running


def gated(row_data, gate_weight, up_weight):
    return (jax.nn.silu(mm(row_data, gate_weight)) * mm(row_data, up_weight)).astype(BF16)


def on_device(
    conv_input,
    conv_kernel,
    conv_gain,
    out_weight,
    moe_input,
    moe_gain,
    expert_gate,
    expert_up,
    expert_down,
    shared_gate,
    shared_up,
    shared_down,
    expert_index,
    routing_weight,
):
    ep_ranks = lax.axis_size("ep")
    tokens, width = moe_input.shape
    slots = 3 * tokens * 2 // (2 * ep_ranks)
    part = slots // CHUNKS
    pieces = 8
    lanes = width // pieces
    tp_index = lax.axis_index("tp").astype(jnp.int32).reshape(1)

    normal, slot_rows, packed = dispatch(
        tp_index, moe_input, moe_gain[None, :], expert_index.T, CHUNKS, slots, ep_ranks, lanes
    )
    block = 8 * pieces * part
    step = block // pieces
    r = jnp.arange(block, dtype=jnp.int32)
    source = (r % step) // part * (pieces * part) + r // step * part + r % part
    perm = (source[:, None] == r[None, :]).astype(BF16)
    perm_t = (source[None, :] == r[:, None]).astype(BF16)

    def exchanged(rows):
        shape = (ep_ranks, pieces * part, lanes)
        moved = lax.all_to_all(rows.reshape(shape), "ep", split_axis=0, concat_axis=0, tiled=True)
        return moved.reshape(rows.shape)

    def gathered(rows):
        half = rows.shape[0] // 2
        back = shifted(rows, "tp", 1)
        ahead = shifted(rows, "tp", -1)
        far_a = shifted(back[:half], "tp", 1)
        far_b = shifted(ahead[half:], "tp", -1)
        return rows, back, ahead, far_a, far_b

    def reduced(own, send_p, send_m, keep_b, keep_a):
        half = keep_b.shape[0]
        got_p = shifted(send_p, "tp", 1)
        got_m = shifted(send_m, "tp", -1)
        last_p = shifted((keep_b.astype(F32) + got_p[:half].astype(F32)).astype(BF16), "tp", 1)
        last_m = shifted((keep_a.astype(F32) + got_m[:half].astype(F32)).astype(BF16), "tp", -1)
        return finish(own, got_p, got_m, last_p, last_m, perm_t, lanes)

    arrived = [exchanged(p) for p in packed]

    reach = conv_kernel.shape[0] - 1
    length = conv_input.shape[0]
    halo_rows = passed_along(conv_input[length - reach :], ("ep", "tp"), 1)
    padded = jnp.concatenate([halo_rows, conv_input], axis=0)
    mixed_rows = depthwise(padded, conv_kernel, length)
    normed = jax.nn.silu(layer_scale(mixed_rows, conv_gain)).astype(BF16)
    conv_out = mm(lax.all_gather(normed, "tp", axis=0, tiled=True), out_weight).astype(BF16)

    spread = [gathered(a) for a in arrived]
    partial = [run_experts(s, perm, expert_gate[0], expert_up[0], expert_down[0]) for s in spread]
    returned = [exchanged(reduced(*p)) for p in partial]

    shared_hidden = gated(normal, shared_gate, shared_up)
    total = mm(shared_hidden, shared_down)
    weights = routing_weight.T
    for k in range(CHUNKS):
        dtype = BF16 if k == CHUNKS - 1 else F32
        total = combine(k, part, slots, slot_rows, weights, returned[k], total, dtype)
    return (conv_out, total)


def solution(mesh):
    in_specs = (
        P(("ep", "tp"), None),
        P(),
        P(),
        P(None, "tp"),
        P(("ep", "tp"), None),
        P(),
        P("ep", None, "tp"),
        P("ep", None, "tp"),
        P("ep", "tp", None),
        P(),
        P(),
        P(),
        P("ep", None),
        P(("ep", "tp"), None),
    )
    out_specs = (P("ep", "tp"), P(("ep", "tp"), None))
    return jax.shard_map(
        on_device, mesh=mesh, in_specs=in_specs, out_specs=out_specs, check_vma=False
    )
```
